32 devices in a mesh: grp: 2 (over y), kv: 4 (over z), tp: 4 (over x, core).
Axes of the slice: x: 2, y: 2, z: 4, core: 2. Of those that a mesh axis runs over, the one named last changes fastest.
Arguments:
- tokens: bfloat16 [176, 6, 4096], P(('grp', 'kv')), parts along dimension 0, may hold values from -6 to 6
- norm_gain: bfloat16 [4096], replicated, may hold values from 0.099609375 to 1.8984375
- w_query: bfloat16 [4096, 2048], P('kv', 'tp'), may hold values from -0.09375 to 0.09375
- w_key: bfloat16 [4096, 2048], P('kv', 'tp'), may hold values from -0.09375 to 0.09375
- w_value: bfloat16 [4096, 2048], P('kv', 'tp'), may hold values from -0.09375 to 0.09375
- w_igate: bfloat16 [4096, 16], P(None, 'tp'), may hold values from -0.09375 to 0.09375
- w_fgate: bfloat16 [4096, 16], P(None, 'tp'), may hold values from -0.09375 to 0.09375
- igate_bias: float32 [16], P('tp'), may hold values from -2 to 2
- fgate_bias: float32 [16], P('tp'), may hold values from 0.5 to 6
- head_gain: bfloat16 [2048], P('tp'), may hold values from 0.099609375 to 1.8984375
- w_out: bfloat16 [2048, 4096], P('tp', 'kv'), may hold values from -0.125 to 0.125
- state_matrix: float32 [176, 16, 128, 128], P(('grp', 'kv'), 'tp'), parts along dimension 0, may hold values from -1.5 to 1.5
- state_norm: float32 [176, 16, 128], P(('grp', 'kv'), 'tp'), parts along dimension 0, may hold values from -4 to 4
- state_max: float32 [176, 16], P(('grp', 'kv'), 'tp'), parts along dimension 0, may hold values from -4 to 4
- prior_keys: bfloat16 [176, 6, 2048], P(('grp', 'kv'), None, 'tp'), parts along dimension 0, may hold values from -6 to 6
- prior_values: bfloat16 [176, 6, 2048], P(('grp', 'kv'), None, 'tp'), parts along dimension 0, may hold values from -6 to 6
- prior_igate: float32 [176, 6, 16], P(('grp', 'kv'), None, 'tp'), parts along dimension 0, may hold values from -4 to 4
- prior_fgate: float32 [176, 6, 16], P(('grp', 'kv'), None, 'tp'), parts along dimension 0, may hold values from 0 to 5
- accepted: int32 [176], P(('grp', 'kv')), parts along dimension 0, may hold values from 0 to 6
Outputs:
- mixed: float32 [176, 6, 4096], P(('grp', 'kv'), None, 'tp'), parts along dimension 0
- new_matrix: float32 [176, 16, 128, 128], P(('grp', 'kv'), 'tp'), parts along dimension 0
- new_norm: float32 [176, 16, 128], P(('grp', 'kv'), 'tp'), parts along dimension 0
- new_max: float32 [176, 16], P(('grp', 'kv'), 'tp'), parts along dimension 0
The draws below stay inside these ranges and needn't reach their ends.
There are 2 independent parts, one for each index of `grp`. The reference program is written for one: setup_inputs(seed, part) draws one part's arguments, and reference() takes and returns one part's arrays. A program takes and returns all parts, laid end to end along the dimension named above; an argument that names none is the same for every part. Nothing has to cross between parts.
Inputs may be any that keep to these rules, and one draw needn't show every extreme that they name: `accepted`: how many of the 6 proposals of the last step were kept, from the first on.
All inputs are finite; a program needn't handle non-finite values.
Results may differ from the reference program's by a relative error of at most 0.019.
Values may be sent and summed in bfloat16 or wider, within the bound.
A program may use at most 128 MiB of HBM per device.

```python
import jax
import jax.numpy as jnp
from jax import lax

D = 4096
HEADS = 16
DK = 128
DV = 128
PROP = 6
SEQS = 88


def with_ends(drawn, own_key, low, high):
    longest = drawn.shape.index(max(drawn.shape))
    spots = []
    for shift in (0, 1):
        where = [jax.random.randint(jax.random.fold_in(own_key, axis), (), 0, length) for axis, length in enumerate(drawn.shape)]
        where[longest] = (where[longest] + shift) % drawn.shape[longest]
        spots.append(tuple(where))
    return drawn.at[spots[0]].set(low).at[spots[1]].set(high)


def block_scale(own_key, shape, shards, smallest, top_value):
    level, own = 1.0, jax.random.fold_in(own_key, 6)
    for axis_at, shards_of in shards:
        draws = jnp.exp(jax.random.uniform(jax.random.fold_in(own, axis_at), (shards_of,), jnp.float32, smallest / len(shards), top_value / len(shards)))
        level = level * jnp.repeat(draws, shape[axis_at] // shards_of).reshape([-1 if axis == axis_at else 1 for axis in range(len(shape))])
    return level


def bell_draw(stream_key, shape, deviation, limit, pieces=(), kind=jnp.bfloat16):
    result = jax.random.normal(stream_key, shape, jnp.float32) * deviation
    if len(pieces) > 0:
        result = block_scale(stream_key, shape, pieces, -0.22, 0.18) * result
    return jnp.clip(result, min=-limit, max=limit).astype(kind)


def setup_inputs(seed: int = 0, part: int = 0) -> dict:
    key_of = jax.random.split(jax.random.key(seed), 20)
    part_splits = jax.random.split(jax.random.fold_in(key_of[19], part), 20)
    tokens = bell_draw(part_splits[0], (SEQS, PROP, D), 1.0, 6.0, ((0, 4),))
    norm_gain = jnp.clip(1.0 + 0.18 * jax.random.normal(key_of[1], (D,), jnp.float32), 0.099609375, 1.8984375).astype(jnp.bfloat16)
    w_query = bell_draw(key_of[2], (D, HEADS * DK), D ** -0.5, 0.09375, ((0, 4), (1, 4)))
    w_key = bell_draw(key_of[3], (D, HEADS * DK), D ** -0.5, 0.09375, ((0, 4), (1, 4)))
    w_value = bell_draw(key_of[4], (D, HEADS * DV), D ** -0.5, 0.09375, ((0, 4), (1, 4)))
    w_igate = bell_draw(key_of[5], (D, HEADS), D ** -0.5, 0.09375, ((1, 4),))
    w_fgate = bell_draw(key_of[6], (D, HEADS), D ** -0.5, 0.09375, ((1, 4),))
    igate_bias = jnp.clip(jax.random.uniform(key_of[7], (HEADS,), jnp.float32, -2.0, 2.0) * block_scale(key_of[7], (HEADS,), ((0, 4),), -0.4, 0.0), -2.0, 2.0)
    fgate_bias = jnp.clip(0.5 + 5.5 * jax.random.uniform(key_of[8], (HEADS,), jnp.float32) ** block_scale(key_of[8], (HEADS,), ((0, 4),), -0.2, 0.2), 0.5, 6.0)
    head_gain = jnp.clip(1.0 + 0.18 * jax.random.normal(key_of[9], (HEADS * DV,), jnp.float32), 0.099609375, 1.8984375).astype(jnp.bfloat16)
    w_out = bell_draw(key_of[10], (HEADS * DV, D), (HEADS * DV) ** -0.5, 0.125, ((0, 4), (1, 4)))
    state_matrix = bell_draw(part_splits[11], (SEQS, HEADS, DK, DV), 0.1, 1.5, ((0, 4), (1, 4)), jnp.float32)
    state_norm = bell_draw(part_splits[12], (SEQS, HEADS, DK), 0.3, 4.0, ((0, 4), (1, 4)), jnp.float32)
    state_max = bell_draw(part_splits[13], (SEQS, HEADS), 1.0, 4.0, ((0, 4), (1, 4)), jnp.float32)
    prior_keys = bell_draw(part_splits[14], (SEQS, PROP, HEADS * DK), 1.0, 6.0, ((0, 4), (2, 4)))
    prior_values = bell_draw(part_splits[15], (SEQS, PROP, HEADS * DV), 1.0, 6.0, ((0, 4), (2, 4)))
    prior_igate = bell_draw(part_splits[16], (SEQS, PROP, HEADS), 1.0, 4.0, ((0, 4), (2, 4)), jnp.float32)
    prior_fgate = jnp.clip(5.0 * jax.random.uniform(part_splits[17], (SEQS, PROP, HEADS), jnp.float32) ** block_scale(part_splits[17], (SEQS, PROP, HEADS), ((0, 4), (2, 4)), -0.2, 0.2), 0.0, 5.0)
    accepted = with_ends(jax.random.randint(part_splits[18], (SEQS,), 0, PROP + 1), jax.random.fold_in(part_splits[18], 1), 0, PROP).astype(jnp.int32)
    return {"tokens": tokens, "norm_gain": norm_gain, "w_query": w_query, "w_key": w_key, "w_value": w_value, "w_igate": w_igate, "w_fgate": w_fgate, "igate_bias": igate_bias, "fgate_bias": fgate_bias, "head_gain": head_gain, "w_out": w_out, "state_matrix": state_matrix, "state_norm": state_norm, "state_max": state_max, "prior_keys": prior_keys, "prior_values": prior_values, "prior_igate": prior_igate, "prior_fgate": prior_fgate, "accepted": accepted}


EPS = 1e-06

def heads_first(array, heads):
    seqs_n, props, width = array.shape
    return array.astype(jnp.float32).reshape(seqs_n, props, heads, width // heads).transpose(0, 2, 1, 3)

def fold_prior(matrix, normer, stabil, keys, values, in_pre, forget_pre, accepted):
    positions = jnp.arange(keys.shape[2], dtype=jnp.int32)
    active_mask = positions[None, None, :] < accepted[:, None, None]
    log_forget = jnp.where(active_mask, jax.nn.log_sigmoid(forget_pre), 0.0)
    in_gate = jnp.where(active_mask, in_pre, -1e+30)
    cum_forget = jnp.cumsum(log_forget, axis=-1)
    total_forget = cum_forget[..., -1]
    weight_log = total_forget[..., None] - cum_forget + in_gate
    new_stabil = jnp.maximum(total_forget + stabil, lax.optimization_barrier(jnp.max(weight_log, axis=-1)))
    carry_scale = jnp.exp(total_forget + stabil - new_stabil)
    weighted_keys = keys * jnp.exp(weight_log - new_stabil[..., None])[..., None]
    new_matrix = carry_scale[..., None, None] * matrix + jnp.einsum('bhtd,bhte->bhde', weighted_keys, values, precision=lax.Precision.HIGHEST)
    new_normer = carry_scale[..., None] * normer + lax.optimization_barrier(jnp.sum(weighted_keys, axis=2))
    return (new_matrix, new_normer, new_stabil)

def read_block(matrix, normer, stabil, query, keys, values, in_pre, forget_pre):
    props = query.shape[2]
    cum_forget = jnp.cumsum(jax.nn.log_sigmoid(forget_pre), axis=-1)
    causal = jnp.tril(jnp.ones((props, props), jnp.bool_))
    log_decay = jnp.where(causal, cum_forget[..., :, None] - cum_forget[..., None, :] + in_pre[..., None, :], -1e+30)
    inter = cum_forget + stabil[..., None]
    row_max = jnp.maximum(inter, lax.optimization_barrier(jnp.max(log_decay, axis=-1)))
    inter_scale = jnp.exp(inter - row_max)
    scores = jnp.einsum('bhtd,bhud->bhtu', query, keys, precision=lax.Precision.HIGHEST)
    scores = scores * jnp.exp(log_decay - row_max[..., None])
    numerator = inter_scale[..., None] * jnp.einsum('bhtd,bhde->bhte', query, matrix, precision=lax.Precision.HIGHEST)
    numerator = numerator + jnp.einsum('bhtu,bhue->bhte', scores, values, precision=lax.Precision.HIGHEST)
    denominator = inter_scale * jnp.einsum('bhtd,bhd->bht', query, normer, precision=lax.Precision.HIGHEST)
    denominator = denominator + lax.optimization_barrier(jnp.sum(scores, axis=-1))
    return numerator / jnp.maximum(jnp.abs(denominator), jnp.exp(-row_max))[..., None]

def head_norm(cell, head_gain):
    seqs_n, heads, props, width = cell.shape
    scaled = cell * lax.rsqrt(lax.optimization_barrier(jnp.mean(cell * cell, axis=-1, keepdims=True)) + EPS)
    scaled = scaled.transpose(0, 2, 1, 3).reshape(seqs_n * props, heads * width)
    return (scaled * head_gain.astype(jnp.float32)).astype(jnp.bfloat16)

def reference(tokens, norm_gain, w_query, w_key, w_value, w_igate, w_fgate, igate_bias, fgate_bias, head_gain, w_out, state_matrix, state_norm, state_max, prior_keys, prior_values, prior_igate, prior_fgate, accepted):
    inputs = tokens.astype(jnp.float32)
    normed = inputs * lax.rsqrt(lax.optimization_barrier(jnp.mean(inputs * inputs, axis=-1, keepdims=True)) + EPS)
    normed = (normed * norm_gain.astype(jnp.float32)).astype(jnp.bfloat16).reshape(SEQS * PROP, D)
    query = jnp.dot(normed, w_query, preferred_element_type=jnp.float32).astype(jnp.bfloat16)
    keys = jnp.dot(normed, w_key, preferred_element_type=jnp.float32).astype(jnp.bfloat16)
    values = jnp.dot(normed, w_value, preferred_element_type=jnp.float32).astype(jnp.bfloat16)
    in_pre = jnp.dot(normed, w_igate, preferred_element_type=jnp.float32) + igate_bias
    forget_pre = jnp.dot(normed, w_fgate, preferred_element_type=jnp.float32) + fgate_bias
    in_pre = in_pre.reshape(SEQS, PROP, HEADS).transpose(0, 2, 1)
    forget_pre = forget_pre.reshape(SEQS, PROP, HEADS).transpose(0, 2, 1)
    new_matrix, new_normer, new_stabil = fold_prior(state_matrix, state_norm, state_max, heads_first(prior_keys, HEADS) * DK ** (-0.5), heads_first(prior_values, HEADS), prior_igate.transpose(0, 2, 1), prior_fgate.transpose(0, 2, 1), accepted)
    cell = read_block(new_matrix, new_normer, new_stabil, heads_first(query.reshape(SEQS, PROP, -1), HEADS), heads_first(keys.reshape(SEQS, PROP, -1), HEADS) * DK ** (-0.5), heads_first(values.reshape(SEQS, PROP, -1), HEADS), in_pre, forget_pre)
    hidden = head_norm(cell, head_gain)
    mixed = jnp.dot(hidden, w_out, preferred_element_type=jnp.float32).reshape(SEQS, PROP, D)
    return (mixed, new_matrix, new_normer, new_stabil)
```

```python
import functools

import jax
import jax.numpy as jnp
from jax import lax
from jax.experimental import pallas as pl
from jax.experimental.pallas import tpu as pltpu
from jax.sharding import PartitionSpec as P

EPS = 1e-06
MESH = pl.DeviceIdType.MESH


def greet_all(kv_size, tp_size):
    z, t = lax.axis_index("kv"), lax.axis_index("tp")
    barrier = pltpu.get_barrier_semaphore()
    for dz in range(kv_size):
        for dt in range(tp_size):
            if dz or dt:
                pl.semaphore_signal(
                    barrier,
                    1,
                    device_id={"kv": lax.rem(z + dz, kv_size), "tp": lax.rem(t + dt, tp_size)},
                    device_id_type=MESH,
                )
    pl.semaphore_wait(barrier, kv_size * tp_size - 1)


def other_at(index, z, kv_size):
    right = kv_size - 1 - z
    near, far = jnp.minimum(z, right), jnp.maximum(z, right)
    single = far - near
    later = index - single
    both = jnp.where(later % 2 == 0, z + near - later // 2, z - near + later // 2)
    lone = jnp.where(right > z, z + far - index, z - far + index)
    return jnp.where(index < single, lone, both)


def merged_away(source, j, kv_size):
    inner = jnp.logical_and(j > 0, j < kv_size - 1)
    return jnp.logical_and(inner, jnp.abs(source - j) == 2)


def row_chunks(rows, count):
    step = -(-(-(-rows // count)) // 8) * 8
    return [(at, min(step, rows - at)) for at in range(0, rows, step)]


def remote(src, dst, send, recv, kv, tp):
    return pltpu.make_async_remote_copy(
        src_ref=src,
        dst_ref=dst,
        send_sem=send,
        recv_sem=recv,
        device_id={"kv": kv, "tp": tp},
        device_id_type=MESH,
    )


def project_kernel(
    kv_size,
    tp_size,
    chunks,
    normed_ref,
    wq_ref,
    wk_ref,
    wv_ref,
    out_ref,
    rows_in,
    weights,
    own_sum,
    partial,
    outgoing,
    incoming,
    merging,
    weight_sem,
    a_send,
    a_recv,
    f_send,
    f_recv,
    b_send,
    b_recv,
    m_recv,
):
    z, t = lax.axis_index("kv"), lax.axis_index("tp")
    depth = weights.shape[0]
    part = depth // tp_size
    width = wq_ref.shape[1]
    others = kv_size - 1
    loads = [
        pltpu.make_async_copy(ref, weights.at[:, pl.ds(at * width, width)], weight_sem.at[at])
        for at, ref in enumerate((wq_ref, wk_ref, wv_ref))
    ]
    for load in loads:
        load.start()
    greet_all(kv_size, tp_size)

    def mine(at):
        return pl.ds(pl.multiple_of(at * part, part), part)

    def first_copy(j, source):
        columns = pl.ds(pl.multiple_of(j * depth + t * part, part), part)
        return remote(
            normed_ref.at[:, columns], rows_in.at[source, :, mine(t)], a_send.at[j], a_recv.at[source], j, t
        )

    def forward_copy(j, source, dt):
        peer = lax.rem(t + dt, tp_size)
        return remote(
            rows_in.at[j, :, mine(source)],
            rows_in.at[j, :, mine(source)],
            f_send.at[j, dt],
            f_recv.at[j, source],
            z,
            peer,
        )

    def start_first(index, carry):
        first_copy(other_at(index, z, kv_size), z).start()
        return carry

    lax.fori_loop(0, others, start_first, 0)
    for load in loads:
        load.wait()
    own_columns = pl.ds(pl.multiple_of(z * depth, depth), depth)
    for at, count in chunks:
        own_sum[pl.ds(at, count), :] = jnp.dot(
            normed_ref[pl.ds(at, count), own_columns], weights[...], preferred_element_type=jnp.float32
        )

    def forward(index, carry):
        j = other_at(index, z, kv_size)
        first_copy(z, j).wait_recv()
        for dt in range(1, tp_size):
            forward_copy(j, t, dt).start()
        return carry

    lax.fori_loop(0, others, forward, 0)

    def merge_copy(j, number, rows):
        way = jnp.where(j > z, 1, 0)
        middle = jnp.where(j > z, z + 1, z - 1)
        return remote(
            outgoing.at[j, rows, :],
            merging.at[way, rows, :],
            b_send.at[j, number],
            m_recv.at[way, number],
            middle,
            t,
        )

    def sum_copy(j, source, number, rows):
        return remote(
            outgoing.at[j, rows, :],
            incoming.at[source, rows, :],
            b_send.at[j, number],
            b_recv.at[source, number],
            j,
            t,
        )

    def unit(number, at, count, index):
        j = other_at(index, z, kv_size)
        way = jnp.where(j > z, 1, 0)
        behind = 2 * z - j
        merges = jnp.logical_and(behind >= 0, behind < kv_size)
        merges = jnp.logical_and(merges, merged_away(behind, j, kv_size))
        if number == 0:
            for dt in range(1, tp_size):
                forward_copy(j, lax.rem(t + dt, tp_size), dt).wait_recv()
        rows = pl.ds(at, count)
        partial[pl.ds(0, count), :] = jnp.dot(
            rows_in[j, rows, :], weights[...], preferred_element_type=jnp.float32
        )

        @pl.when(merges)
        def _():
            merge_copy(j, number, rows).wait_recv()
            partial[pl.ds(0, count), :] += merging[way, rows, :].astype(jnp.float32)

        outgoing[j, rows, :] = partial[pl.ds(0, count), :].astype(jnp.bfloat16)
        away = merged_away(z, j, kv_size)

        @pl.when(away)
        def _():
            merge_copy(j, number, rows).start()

        @pl.when(jnp.logical_not(away))
        def _():
            sum_copy(j, z, number, rows).start()

    for number, (at, count) in enumerate(chunks):

        def run(index, carry, number=number, at=at, count=count):
            unit(number, at, count, index)
            return carry

        lax.fori_loop(0, others, run, 0)

    for number, (at, count) in enumerate(chunks):
        rows = pl.ds(at, count)

        def add(index, carry, rows=rows, number=number):
            j = other_at(index, z, kv_size)

            @pl.when(jnp.logical_not(merged_away(j, z, kv_size)))
            def _():
                sum_copy(z, j, number, rows).wait_recv()
                own_sum[rows, :] += incoming[j, rows, :].astype(jnp.float32)

            return carry

        lax.fori_loop(0, others, add, 0)
        out_ref[rows, :] = own_sum[rows, :].astype(jnp.bfloat16)

    def drain(index, carry):
        j = other_at(index, z, kv_size)
        first_copy(j, z).wait_send()
        for dt in range(1, tp_size):
            forward_copy(j, t, dt).wait_send()
        for number, (at, count) in enumerate(chunks):
            sum_copy(j, z, number, pl.ds(at, count)).wait_send()
        return carry

    lax.fori_loop(0, others, drain, 0)


def project(normed_rows, w_query, w_key, w_value, kv_size, tp_size):
    rows, width = normed_rows.shape
    depth = width // kv_size
    columns = 3 * w_query.shape[1]
    chunks = row_chunks(rows, 3)
    sem = pltpu.SemaphoreType.DMA
    hbm = pl.BlockSpec(memory_space=pl.ANY)
    return pl.pallas_call(
        functools.partial(project_kernel, kv_size, tp_size, chunks),
        out_shape=jax.ShapeDtypeStruct((rows, columns), jnp.bfloat16),
        in_specs=[pl.BlockSpec(memory_space=pltpu.VMEM), hbm, hbm, hbm],
        out_specs=pl.BlockSpec(memory_space=pltpu.VMEM),
        scratch_shapes=[
            pltpu.VMEM((kv_size, rows, depth), jnp.bfloat16),
            pltpu.VMEM((depth, columns), jnp.bfloat16),
            pltpu.VMEM((rows, columns), jnp.float32),
            pltpu.VMEM((chunks[0][1], columns), jnp.float32),
            pltpu.VMEM((kv_size, rows, columns), jnp.bfloat16),
            pltpu.VMEM((kv_size, rows, columns), jnp.bfloat16),
            pltpu.VMEM((2, rows, columns), jnp.bfloat16),
            sem((3,)),
            sem((kv_size,)),
            sem((kv_size,)),
            sem((kv_size, tp_size)),
            sem((kv_size, tp_size)),
            sem((kv_size, len(chunks))),
            sem((kv_size, len(chunks))),
            sem((2, len(chunks))),
        ],
        compiler_params=pltpu.CompilerParams(
            collective_id=0, has_side_effects=True, vmem_limit_bytes=60 * 1024 * 1024
        ),
    )(normed_rows, w_query, w_key, w_value)


def output_kernel(
    kv_size,
    tp_size,
    stages,
    hidden_ref,
    w_ref,
    out_ref,
    hidden_in,
    weights,
    sums,
    landed,
    *rest,
):
    halves = rest[: 2 * stages]
    weight_sem, h_send, h_recv, r_send, r_recv, o_send, o_recv, outgoing = rest[2 * stages :]
    z, t = lax.axis_index("kv"), lax.axis_index("tp")
    others = kv_size - 1
    width = weights.shape[1]
    piece = width // tp_size
    load = pltpu.make_async_copy(w_ref, weights, weight_sem.at[0])
    load.start()
    greet_all(kv_size, tp_size)

    def hidden_copy(j, source):
        return remote(hidden_ref, hidden_in.at[source], h_send.at[j], h_recv.at[source], j, t)

    def start_hidden(index, carry):
        hidden_copy(other_at(index, z, kv_size), z).start()
        return carry

    lax.fori_loop(0, others, start_hidden, 0)
    load.wait()

    def half_copy(j, stage):
        peer = jnp.bitwise_xor(t, 1 << stage)
        return remote(
            halves[2 * stage].at[j],
            halves[2 * stage + 1].at[j],
            r_send.at[j, stage],
            r_recv.at[j, stage],
            z,
            peer,
        )

    def split(j, stage, low, high):
        bit = jnp.bitwise_and(lax.shift_right_logical(t, stage), 1)

        @pl.when(bit == 0)
        def _():
            halves[2 * stage][j] = high().astype(jnp.bfloat16)

        @pl.when(bit == 1)
        def _():
            halves[2 * stage][j] = low().astype(jnp.bfloat16)

        half_copy(j, stage).start()

    def bit_of(stage):
        return jnp.bitwise_and(lax.shift_right_logical(t, stage), 1)

    def first_stage(j, block):
        sums[j] = jnp.dot(block, weights[...], preferred_element_type=jnp.float32)
        split(
            j,
            0,
            lambda: sums[j, :, pl.ds(0, width // 2)],
            lambda: sums[j, :, pl.ds(width // 2, width // 2)],
        )

    def each(function):
        def run(index, carry):
            function(jnp.where(index == others, z, other_at(jnp.minimum(index, others - 1), z, kv_size)))
            return carry

        lax.fori_loop(0, kv_size, run, 0)

    first_stage(z, hidden_ref[...])

    def near_first(index, carry):
        j = other_at(others - 1 - index, z, kv_size)
        hidden_copy(z, j).wait_recv()
        first_stage(j, hidden_in[j])
        return carry

    lax.fori_loop(0, others, near_first, 0)

    offset = 0
    for stage in range(stages):
        size = width >> (stage + 1)
        offset = offset + bit_of(stage) * size

        def gather(j, stage=stage, size=size, offset=offset):
            half_copy(j, stage).wait_recv()
            kept = pl.ds(pl.multiple_of(offset, size), size)
            sums[j, :, kept] += halves[2 * stage + 1][j].astype(jnp.float32)
            if stage + 1 < stages:
                small = size // 2
                split(
                    j,
                    stage + 1,
                    lambda: sums[j, :, pl.ds(pl.multiple_of(offset, small), small)],
                    lambda: sums[j, :, pl.ds(pl.multiple_of(offset + small, small), small)],
                )
            else:
                outgoing[j] = sums[j, :, kept].astype(jnp.bfloat16)

                @pl.when(jnp.logical_or(j != z, t != z))
                def _():
                    final_copy(j).start()

        def final_copy(j):
            return remote(outgoing.at[j], landed.at[t], o_send.at[j], o_recv.at[t], j, z)

        each(gather)

    for sender in range(tp_size):
        at = sum(((sender >> stage) & 1) * (width >> (stage + 1)) for stage in range(stages))
        columns = pl.ds(at, piece)
        local = jnp.logical_and(z == t, t == sender)

        @pl.when(local)
        def _(columns=columns):
            out_ref[:, columns] = outgoing[z].astype(jnp.float32)

        @pl.when(jnp.logical_not(local))
        def _(columns=columns, sender=sender):
            remote(landed.at[sender], landed.at[sender], o_send.at[0], o_recv.at[sender], z, t).wait_recv()
            out_ref[:, columns] = landed[sender].astype(jnp.float32)

    def drain(index, carry):
        hidden_copy(other_at(index, z, kv_size), z).wait_send()
        return carry

    lax.fori_loop(0, others, drain, 0)

    def drain_each(j):
        for stage in range(stages):
            half_copy(j, stage).wait_send()

        @pl.when(jnp.logical_or(j != z, t != z))
        def _():
            remote(outgoing.at[j], landed.at[t], o_send.at[j], o_recv.at[t], j, z).wait_send()

    each(drain_each)


def output(hidden, w_out, kv_size, tp_size):
    rows, heads_width = hidden.shape
    width = w_out.shape[1]
    stages = tp_size.bit_length() - 1
    sem = pltpu.SemaphoreType.DMA
    halves = []
    for stage in range(stages):
        halves += [pltpu.VMEM((kv_size, rows, width >> (stage + 1)), jnp.bfloat16)] * 2
    piece = width // tp_size
    return pl.pallas_call(
        functools.partial(output_kernel, kv_size, tp_size, stages),
        out_shape=jax.ShapeDtypeStruct((rows, width), jnp.float32),
        in_specs=[pl.BlockSpec(memory_space=pltpu.VMEM), pl.BlockSpec(memory_space=pl.ANY)],
        out_specs=pl.BlockSpec(memory_space=pltpu.VMEM),
        scratch_shapes=[
            pltpu.VMEM((kv_size, rows, heads_width), jnp.bfloat16),
            pltpu.VMEM((heads_width, width), jnp.bfloat16),
            pltpu.VMEM((kv_size, rows, width), jnp.float32),
            pltpu.VMEM((tp_size, rows, piece), jnp.bfloat16),
            *halves,
            sem((1,)),
            sem((kv_size,)),
            sem((kv_size,)),
            sem((kv_size, stages)),
            sem((kv_size, stages)),
            sem((kv_size,)),
            sem((tp_size,)),
            pltpu.VMEM((kv_size, rows, piece), jnp.bfloat16),
        ],
        compiler_params=pltpu.CompilerParams(
            collective_id=1, has_side_effects=True, vmem_limit_bytes=60 * 1024 * 1024
        ),
    )(hidden, w_out)


def kernels_fit(kv_size, tp_size, width, out_width):
    powers = kv_size == tp_size and tp_size >= 2 and tp_size & (tp_size - 1) == 0
    lanes = 128 * tp_size
    return powers and (width // kv_size) % lanes == 0 and out_width % lanes == 0


def reduce_tiles(partial, axis_name, axis):
    size = lax.psum(1, axis_name)
    shape = partial.shape
    split = partial.astype(jnp.bfloat16).reshape(
        shape[:axis] + (size, shape[axis] // size) + shape[axis + 1 :]
    )
    split = jnp.moveaxis(split, axis, 0)
    got = lax.all_to_all(split, axis_name, split_axis=0, concat_axis=0, tiled=True)
    return jnp.sum(got.astype(jnp.float32), axis=0)


def bf_dot(spec, left, right):
    return jnp.einsum(
        spec,
        left.astype(jnp.bfloat16),
        right.astype(jnp.bfloat16),
        preferred_element_type=jnp.float32,
    )


def heads_first(array, heads):
    seqs_n, props, width = array.shape
    return (
        array.astype(jnp.float32)
        .reshape(seqs_n, props, heads, width // heads)
        .transpose(0, 2, 1, 3)
    )


def fold_prior(matrix, normer, stabil, keys, values, in_pre, forget_pre, accepted):
    positions = jnp.arange(keys.shape[2], dtype=jnp.int32)
    active_mask = positions[None, None, :] < accepted[:, None, None]
    log_forget = jnp.where(active_mask, jax.nn.log_sigmoid(forget_pre), 0.0)
    in_gate = jnp.where(active_mask, in_pre, -1e30)
    cum_forget = jnp.cumsum(log_forget, axis=-1)
    total_forget = cum_forget[..., -1]
    weight_log = total_forget[..., None] - cum_forget + in_gate
    new_stabil = jnp.maximum(total_forget + stabil, jnp.max(weight_log, axis=-1))
    carry_scale = jnp.exp(total_forget + stabil - new_stabil)
    weighted_keys = keys * jnp.exp(weight_log - new_stabil[..., None])[..., None]
    new_matrix = carry_scale[..., None, None] * matrix + bf_dot(
        "bhtd,bhte->bhde", weighted_keys, values
    )
    new_normer = carry_scale[..., None] * normer + jnp.sum(weighted_keys, axis=2)
    return (new_matrix, new_normer, new_stabil)


def read_block(matrix, normer, stabil, query, keys, values, in_pre, forget_pre):
    props = query.shape[2]
    cum_forget = jnp.cumsum(jax.nn.log_sigmoid(forget_pre), axis=-1)
    causal = jnp.tril(jnp.ones((props, props), jnp.bool_))
    log_decay = jnp.where(
        causal, cum_forget[..., :, None] - cum_forget[..., None, :] + in_pre[..., None, :], -1e30
    )
    inter = cum_forget + stabil[..., None]
    row_max = jnp.maximum(inter, jnp.max(log_decay, axis=-1))
    inter_scale = jnp.exp(inter - row_max)
    scores = bf_dot("bhtd,bhud->bhtu", query, keys)
    scores = scores * jnp.exp(log_decay - row_max[..., None])
    numerator = inter_scale[..., None] * bf_dot(
        "bhtd,bhde->bhte", query, matrix
    )
    numerator = numerator + bf_dot(
        "bhtu,bhue->bhte", scores, values
    )
    denominator = inter_scale * jnp.sum(query * normer[:, :, None, :], axis=-1)
    denominator = denominator + jnp.sum(scores, axis=-1)
    return numerator / jnp.maximum(jnp.abs(denominator), jnp.exp(-row_max))[..., None]


def head_norm(cell, head_gain):
    seqs_n, heads, props, width = cell.shape
    scaled = cell * lax.rsqrt(jnp.mean(cell * cell, axis=-1, keepdims=True) + EPS)
    scaled = scaled.transpose(0, 2, 1, 3).reshape(seqs_n * props, heads * width)
    return (scaled * head_gain.astype(jnp.float32)).astype(jnp.bfloat16)


def body(
    tokens,
    norm_gain,
    w_query,
    w_key,
    w_value,
    w_igate,
    w_fgate,
    igate_bias,
    fgate_bias,
    head_gain,
    w_out,
    state_matrix,
    state_norm,
    state_max,
    prior_keys,
    prior_values,
    prior_igate,
    prior_fgate,
    accepted,
):
    seq_count, props, width = tokens.shape
    local_heads = state_matrix.shape[1]
    key_size = state_matrix.shape[2]
    row_count = seq_count * props
    inputs = tokens.astype(jnp.float32)
    normed = inputs * lax.rsqrt(jnp.mean(inputs * inputs, axis=-1, keepdims=True) + EPS)
    normed_rows = (
        (normed * norm_gain.astype(jnp.float32)).astype(jnp.bfloat16).reshape(row_count, width)
    )
    query_width = w_query.shape[1]
    kv_size, tp_size = lax.axis_size("kv"), lax.axis_size("tp")
    own_kernels = kernels_fit(kv_size, tp_size, width, w_out.shape[1])
    if own_kernels:
        summed = project(normed_rows, w_query, w_key, w_value, kv_size, tp_size)
    else:
        combined = jnp.concatenate([w_query, w_key, w_value], axis=1)
        received = lax.all_to_all(normed_rows, "kv", split_axis=1, concat_axis=0, tiled=True)
        summed = reduce_tiles(
            jnp.dot(received, combined, preferred_element_type=jnp.float32), "kv", 0
        )
    query_sum = summed[:, :query_width]
    key_sum = summed[:, query_width : 2 * query_width]
    value_sum = summed[:, 2 * query_width :]
    query = query_sum.astype(jnp.bfloat16).reshape(seq_count, props, -1)
    keys = key_sum.astype(jnp.bfloat16).reshape(seq_count, props, -1)
    values = value_sum.astype(jnp.bfloat16).reshape(seq_count, props, -1)
    in_pre = jnp.dot(normed_rows, w_igate, preferred_element_type=jnp.float32) + igate_bias
    forget_pre = jnp.dot(normed_rows, w_fgate, preferred_element_type=jnp.float32) + fgate_bias
    in_pre = in_pre.reshape(seq_count, props, local_heads).transpose(0, 2, 1)
    forget_pre = forget_pre.reshape(seq_count, props, local_heads).transpose(0, 2, 1)
    new_matrix, new_normer, new_stabil = fold_prior(
        state_matrix,
        state_norm,
        state_max,
        heads_first(prior_keys, local_heads) * key_size ** (-0.5),
        heads_first(prior_values, local_heads),
        prior_igate.transpose(0, 2, 1),
        prior_fgate.transpose(0, 2, 1),
        accepted,
    )
    cell = read_block(
        new_matrix,
        new_normer,
        new_stabil,
        heads_first(query, local_heads),
        heads_first(keys, local_heads) * key_size ** (-0.5),
        heads_first(values, local_heads),
        in_pre,
        forget_pre,
    )
    hidden = head_norm(cell, head_gain)
    if own_kernels:
        mixed = output(hidden, w_out, kv_size, tp_size)
    else:
        partial_out = jnp.dot(
            hidden,
            lax.all_gather(w_out, "kv", axis=1, tiled=True),
            preferred_element_type=jnp.float32,
        )
        mixed = reduce_tiles(partial_out, "tp", 1)
    return (mixed.reshape(seq_count, props, -1), new_matrix, new_normer, new_stabil)


def solution(mesh):
    return jax.shard_map(
        body,
        mesh=mesh,
        in_specs=(
            P(("grp", "kv"), None, None),
            P(),
            P("kv", "tp"),
            P("kv", "tp"),
            P("kv", "tp"),
            P(None, "tp"),
            P(None, "tp"),
            P("tp"),
            P("tp"),
            P("tp"),
            P("tp", "kv"),
            P(("grp", "kv"), "tp", None, None),
            P(("grp", "kv"), "tp", None),
            P(("grp", "kv"), "tp"),
            P(("grp", "kv"), None, "tp"),
            P(("grp", "kv"), None, "tp"),
            P(("grp", "kv"), None, "tp"),
            P(("grp", "kv"), None, "tp"),
            P(("grp", "kv")),
        ),
        out_specs=(
            P(("grp", "kv"), None, "tp"),
            P(("grp", "kv"), "tp", None, None),
            P(("grp", "kv"), "tp", None),
            P(("grp", "kv"), "tp"),
        ),
        check_vma=False,
    )
```

```python
import functools

import jax
import jax.numpy as jnp
from jax import lax
from jax.experimental import pallas as pl
from jax.experimental.pallas import tpu as pltpu
from jax.sharding import PartitionSpec as P

EPS = 1e-06
MESH = pl.DeviceIdType.MESH


def greet_all(kv_size, tp_size):
    z, t = lax.axis_index("kv"), lax.axis_index("tp")
    barrier = pltpu.get_barrier_semaphore()
    for dz in range(kv_size):
        for dt in range(tp_size):
            if dz or dt:
                pl.semaphore_signal(
                    barrier,
                    1,
                    device_id={"kv": lax.rem(z + dz, kv_size), "tp": lax.rem(t + dt, tp_size)},
                    device_id_type=MESH,
                )
    pl.semaphore_wait(barrier, kv_size * tp_size - 1)


def other_at(index, z, kv_size):
    right = kv_size - 1 - z
    near, far = jnp.minimum(z, right), jnp.maximum(z, right)
    single = far - near
    later = index - single
    both = jnp.where(later % 2 == 0, z + near - later // 2, z - near + later // 2)
    lone = jnp.where(right > z, z + far - index, z - far + index)
    return jnp.where(index < single, lone, both)


def looked_up(table, *at):
    if not at:
        return table
    picked = looked_up(table[0], *at[1:])
    for index in range(1, len(table)):
        picked = jnp.where(at[0] == index, looked_up(table[index], *at[1:]), picked)
    return picked


def send_order(kv_size):
    def merged(source, j):
        return 0 < j < kv_size - 1 and abs(source - j) == 2

    def rank(z, j):
        behind = 2 * z - j
        waits = 0 <= behind < kv_size and merged(behind, j)
        return (waits, not merged(z, j), -abs(z - j), j)

    return [
        sorted((j for j in range(kv_size) if j != z), key=functools.partial(rank, z))
        for z in range(kv_size)
    ]


def merged_away(source, j, kv_size):
    inner = jnp.logical_and(j > 0, j < kv_size - 1)
    return jnp.logical_and(inner, jnp.abs(source - j) == 2)


def remote(src, dst, send, recv, kv, tp):
    return pltpu.make_async_remote_copy(
        src_ref=src,
        dst_ref=dst,
        send_sem=send,
        recv_sem=recv,
        device_id={"kv": kv, "tp": tp},
        device_id_type=MESH,
    )


def log_sigmoid(x):
    return jnp.minimum(x, 0.0) - jnp.log1p(jnp.exp(-jnp.abs(x)))


def step_kernel(sizes, *refs):
    kv_size, tp_size, seqs, props, heads = sizes
    (
        tokens_hbm, gain_ref, wq_hbm, wk_hbm, wv_hbm, wi_ref, wf_ref, ibias_ref, fbias_ref,
        head_gain_ref, wo_hbm, matrix_hbm, norm_ref, max_ref, keys_hbm, values_hbm,
        prior_i_ref, prior_f_ref, accepted_ref,
        out_ref, new_matrix, new_norm_ref, new_max_ref,
        tokens, normed, rows_in, weights, own_sum, partial, outgoing, incoming, merging,
        keys, values, matrix, read_matrix, stacked, columns_of, max_of,
        w_out, hidden_in, sums, outward, landed, *rest,
    ) = refs
    stages = tp_size.bit_length() - 1
    halves = rest[: 2 * stages]
    (
        local_sem, state_sem, a_send, a_recv, f_send, f_recv, b_send, b_recv, m_recv,
        h_send, h_recv, r_send, r_recv, o_send, o_recv,
    ) = rest[2 * stages :]
    z, t = lax.axis_index("kv"), lax.axis_index("tp")
    others = kv_size - 1
    groups = normed.shape[0]
    rows = props * 8
    depth = weights.shape[0]
    part = depth // tp_size
    width = wq_hbm.shape[1]
    key_size = width // heads
    out_width = w_out.shape[1]
    piece = out_width // tp_size
    f32, bf16 = jnp.float32, jnp.bfloat16

    def live_seqs(group):
        return min(8, seqs - 8 * group)

    def eight(block):
        missing = 8 - block.shape[0]
        if missing:
            block = jnp.concatenate([block, jnp.zeros((missing, block.shape[1]), f32)], axis=0)
        return block

    def column(at, size):
        return pl.ds(pl.multiple_of(at, 128), size)

    token_load = pltpu.make_async_copy(tokens_hbm, tokens, local_sem.at[0])
    weight_loads = [
        pltpu.make_async_copy(ref, weights.at[:, pl.ds(at * width, width)], local_sem.at[1 + at])
        for at, ref in enumerate((wq_hbm, wk_hbm, wv_hbm))
    ]
    key_load = pltpu.make_async_copy(keys_hbm, keys, local_sem.at[4])
    value_load = pltpu.make_async_copy(values_hbm, values, local_sem.at[5])
    out_load = pltpu.make_async_copy(wo_hbm, w_out, local_sem.at[6])

    def state_load(group):
        part_of = pl.ds(8 * group, live_seqs(group))
        return pltpu.make_async_copy(matrix_hbm.at[part_of], matrix.at[part_of], state_sem.at[group])

    token_load.start()
    for load in weight_loads:
        load.start()
    key_load.start()
    value_load.start()
    for group in range(groups):
        state_load(group).start()
    out_load.start()
    greet_all(kv_size, tp_size)

    def mine(at):
        return column(at * part, part)

    def first_copy(group, j, source):
        return remote(
            normed.at[group, :, column(j * depth + t * part, part)],
            rows_in.at[source, group, :, mine(t)],
            a_send.at[group, j],
            a_recv.at[group, source],
            j,
            t,
        )

    def forward_copy(group, j, at, stage):
        source = jnp.bitwise_xor(t, at)
        block = rows_in.at[j, group, :, mine(source)]
        peer = jnp.bitwise_xor(t, 1 << stage)
        return remote(
            block, block, f_send.at[group, j, at, stage], f_recv.at[group, j, source], z, peer
        )

    def forwards():
        held = [0]
        for stage in reversed(range(stages)):
            yield stage, list(held)
            held += [at ^ (1 << stage) for at in held]

    def merge_copy(group, j):
        way = jnp.where(j > z, 1, 0)
        middle = jnp.where(j > z, z + 1, z - 1)
        return remote(
            outgoing.at[j, group],
            merging.at[way, group],
            b_send.at[group, j],
            m_recv.at[group, way],
            middle,
            t,
        )

    def sum_copy(group, j, source):
        return remote(
            outgoing.at[j, group],
            incoming.at[source, group],
            b_send.at[group, j],
            b_recv.at[group, source],
            j,
            t,
        )

    def hidden_copy(group, j, source):
        return remote(
            hidden_in.at[group, z],
            hidden_in.at[group, source],
            h_send.at[group, j],
            h_recv.at[group, source],
            j,
            t,
        )

    def half_copy(group, stage, j):
        peer = jnp.bitwise_xor(t, 1 << stage)
        return remote(
            halves[2 * stage].at[group, j],
            halves[2 * stage + 1].at[group, j],
            r_send.at[group, stage, j],
            r_recv.at[group, stage, j],
            z,
            peer,
        )

    def final_copy(group, j):
        return remote(
            outward.at[group, j],
            landed.at[group, t],
            o_send.at[group, j],
            o_recv.at[group, t],
            j,
            z,
        )

    def each_other(function):
        def run(index, carry):
            function(other_at(index, z, kv_size))
            return carry

        lax.fori_loop(0, others, run, 0)

    gain_rows = gain_ref[...].astype(f32)
    gain = jnp.concatenate([gain_rows[at : at + 1] for at in range(gain_rows.shape[0])], axis=1)

    def normalize(group):
        for pair in range(props // 2):
            done = []
            for at in (2 * pair, 2 * pair + 1):
                x = eight(tokens[at, pl.ds(8 * group, live_seqs(group)), :].astype(f32))
                scale = lax.rsqrt(jnp.mean(x * x, axis=-1, keepdims=True) + EPS)
                done.append(x * scale * gain)
            normed[group, pl.ds(16 * pair, 16), :] = jnp.concatenate(done, axis=0).astype(bf16)

    def start_rows(group):
        each_other(lambda j: first_copy(group, j, z).start())

    def forward_rows(group):
        def first(j):
            first_copy(group, z, j).wait_recv()
            for stage in reversed(range(stages)):
                forward_copy(group, j, 0, stage).start()

        def later(j):
            for stage, held in forwards():
                for at in held[1:]:
                    forward_copy(group, j, at, stage).wait_recv()
                    forward_copy(group, j, at, stage).start()

        each_other(first)
        each_other(later)

    def own_part(group):
        own_sum[group] = jnp.dot(
            normed[group, :, column(z * depth, depth)], weights[...], preferred_element_type=f32
        )

    def send_sums(group):
        passed_on = {at for _, held in forwards() for at in held}
        waited_later = [at for at in range(1, tp_size) if at not in passed_on]

        def unit(j):
            way = jnp.where(j > z, 1, 0)
            behind = 2 * z - j
            merges = jnp.logical_and(behind >= 0, behind < kv_size)
            merges = jnp.logical_and(merges, merged_away(behind, j, kv_size))
            for at in waited_later:
                forward_copy(group, j, at, 0).wait_recv()
            partial[...] = jnp.dot(rows_in[j, group], weights[...], preferred_element_type=f32)

            @pl.when(merges)
            def _():
                merge_copy(group, j).wait_recv()
                partial[...] += merging[way, group].astype(f32)

            outgoing[j, group] = partial[...].astype(bf16)
            away = merged_away(z, j, kv_size)

            @pl.when(away)
            def _():
                merge_copy(group, j).start()

            @pl.when(jnp.logical_not(away))
            def _():
                sum_copy(group, j, z).start()

        order = send_order(kv_size)

        def run(index, carry):
            unit(looked_up(order, z, index))
            return carry

        lax.fori_loop(0, others, run, 0)

    def fold_weights():
        stacked[...] = jnp.zeros_like(stacked)
        accepted = accepted_ref[...]
        total = jnp.zeros((heads, seqs), f32)
        sums_of, gates = [], []
        for at in range(props):
            live = jnp.broadcast_to(at < accepted, (heads, seqs))
            total = total + jnp.where(live, log_sigmoid(prior_f_ref[at]), 0.0)
            sums_of.append(total)
            gates.append(jnp.where(live, prior_i_ref[at], -1e30))
        logs = [total - b + gate for b, gate in zip(sums_of, gates)]
        top = functools.reduce(jnp.maximum, logs)
        carried = total + max_ref[...]
        new_max = jnp.maximum(carried, top)
        new_max_ref[...] = new_max
        lanes = pl.ds(0, seqs)
        for at, log in enumerate(logs):
            stacked[0, pl.ds(8 * at, heads), lanes] = jnp.exp(log - new_max)
        stacked[0, pl.ds(8 * props, heads), lanes] = jnp.exp(carried - new_max)
        stacked[1, pl.ds(0, heads), lanes] = new_max
        columns_of[...] = stacked[0].T
        max_of[...] = stacked[1].T

    def fold(group):
        state_load(group).wait()
        live = live_seqs(group)
        here = pl.ds(8 * group, live)
        row_of = lax.broadcasted_iota(jnp.int32, (rows, 1), 0) % 8
        table = columns_of[pl.ds(8 * group, 8), :]
        for head in range(heads):
            lanes = pl.ds(head * key_size, key_size)
            weighted, seen = [], []
            for at in range(props):
                key = eight(keys[at, here, lanes].astype(f32)) * key_size**-0.5
                weighted.append(key * table[:, 8 * at + head : 8 * at + head + 1])
                seen.append(eight(values[at, here, lanes].astype(f32)))
            carry = table[:, 8 * props + head : 8 * props + head + 1]
            normer = carry[:live] * norm_ref[here, head, :]
            new_norm_ref[here, head, :] = normer + sum(weighted)[:live]
            left = jnp.concatenate(weighted, axis=0).astype(bf16)
            value = jnp.concatenate(seen, axis=0)
            spread = jnp.concatenate(
                [jnp.where(row_of == s, value, 0.0).astype(bf16) for s in range(live)], axis=1
            )
            added = lax.dot_general(
                left, spread, (((0,), (0,)), ((), ())), preferred_element_type=f32
            )
            for s in range(live):
                fresh = carry[s : s + 1] * matrix[8 * group + s, head]
                fresh = fresh + added[:, s * key_size : (s + 1) * key_size]
                new_matrix[8 * group + s, head] = fresh
                read_matrix[group, head, :, pl.ds(s * key_size, key_size)] = fresh.astype(bf16)

    def read(group):
        def add(j):
            @pl.when(jnp.logical_not(merged_away(j, z, kv_size)))
            def _():
                sum_copy(group, z, j).wait_recv()
                own_sum[group] += incoming[j, group].astype(f32)

        each_other(add)
        live = live_seqs(group)
        rows_of_seq = lax.broadcasted_iota(jnp.int32, (8, 1), 0)
        contract = (((1,), (1,)), ((), ()))
        in_pre = lax.dot_general(normed[group], wi_ref[...], contract, preferred_element_type=f32)
        forget = lax.dot_general(normed[group], wf_ref[...], contract, preferred_element_type=f32)
        in_pre = in_pre + ibias_ref[...]
        forget = log_sigmoid(forget + fbias_ref[...])
        steps = range(props)
        gate = [in_pre[8 * at : 8 * at + 8] for at in steps]
        total, b = jnp.zeros((8, heads), f32), []
        for at in steps:
            total = total + forget[8 * at : 8 * at + 8]
            b.append(total)
        top = max_of[pl.ds(8 * group, 8), :][:, :heads]
        decay, inter, floor = {}, [], []
        for at in steps:
            logs = [b[at] - b[u] + gate[u] for u in range(at + 1)]
            row_max = functools.reduce(jnp.maximum, logs, b[at] + top)
            inter.append(jnp.exp(b[at] + top - row_max))
            floor.append(jnp.exp(-row_max))
            for u in range(at + 1):
                decay[at, u] = jnp.exp(logs[u] - row_max)
        hidden = []
        for head in range(heads):
            one = slice(head, head + 1)

            def rounded(kind, head=head):
                lanes = pl.ds(kind * width + head * key_size, key_size)
                return own_sum[group, :, lanes].astype(bf16)

            def by_step(array):
                array = array.astype(f32)
                return [array[8 * at : 8 * at + 8] for at in steps]

            query_rows = rounded(0)
            query, key, value = by_step(query_rows), by_step(rounded(1)), by_step(rounded(2))
            held = live * key_size
            inward = jnp.dot(
                query_rows, read_matrix[group, head, :, pl.ds(0, held)], preferred_element_type=f32
            )
            normer = eight(new_norm_ref[pl.ds(8 * group, live), head, :])
            done = []
            for at in steps:
                picked = jnp.zeros((8, key_size), f32)
                for s in range(live):
                    block = inward[8 * at : 8 * at + 8, s * key_size : (s + 1) * key_size]
                    picked = jnp.where(rows_of_seq == s, block, picked)
                scale = inter[at][:, one]
                numerator = scale * picked
                denominator = scale * jnp.sum(query[at] * normer, axis=-1, keepdims=True)
                for u in range(at + 1):
                    score = jnp.sum(query[at] * key[u], axis=-1, keepdims=True) * key_size**-0.5
                    score = score * decay[at, u][:, one]
                    numerator = numerator + score * value[u]
                    denominator = denominator + score
                cell = numerator / jnp.maximum(jnp.abs(denominator), floor[at][:, one])
                mean = jnp.mean(cell * cell, axis=-1, keepdims=True)
                head_scale = head_gain_ref[pl.ds(head, 1), :].astype(f32)
                done.append(cell * lax.rsqrt(mean + EPS) * head_scale)
            hidden.append(jnp.concatenate(done, axis=0).astype(bf16))
        for head in range(heads):
            hidden_in[group, z, :, pl.ds(head * key_size, key_size)] = hidden[head]
        each_other(lambda j: hidden_copy(group, j, z).start())

    def bit_of(stage):
        return jnp.bitwise_and(lax.shift_right_logical(t, stage), 1)

    def kept_at(stage):
        return sum(bit_of(at) * (out_width >> (at + 1)) for at in range(stage))

    def split(group, stage, j):
        half = out_width >> (stage + 1)
        away = kept_at(stage) + (1 - bit_of(stage)) * half
        halves[2 * stage][group, j] = sums[group, j, :, column(away, half)].astype(bf16)
        half_copy(group, stage, j).start()

    def each_near(function):
        def run(index, carry):
            other = other_at(jnp.minimum(others - index, others - 1), z, kv_size)
            function(jnp.where(index == 0, z, other))
            return carry

        lax.fori_loop(0, kv_size, run, 0)

    def multiply(group):
        def one(j):
            @pl.when(j != z)
            def _():
                hidden_copy(group, z, j).wait_recv()

            sums[group, j] = jnp.dot(hidden_in[group, j], w_out[...], preferred_element_type=f32)
            split(group, 0, j)

        each_near(one)

    def reduce(group, stage):
        def one(j):
            half_copy(group, stage, j).wait_recv()
            kept = column(kept_at(stage + 1), out_width >> (stage + 1))
            sums[group, j, :, kept] += halves[2 * stage + 1][group, j].astype(f32)
            if stage + 1 < stages:
                split(group, stage + 1, j)
                return
            outward[group, j] = sums[group, j, :, kept].astype(bf16)

            @pl.when(jnp.logical_or(j != z, t != z))
            def _():
                final_copy(group, j).start()

        each_near(one)

    def finish(group):
        live = live_seqs(group)
        for sender in range(tp_size):
            at = sum(((sender >> stage) & 1) * (out_width >> (stage + 1)) for stage in range(stages))
            local = jnp.logical_and(z == t, t == sender)

            @pl.when(local)
            def _(sender=sender):
                landed[group, sender] = outward[group, z]

            @pl.when(jnp.logical_not(local))
            def _(sender=sender):
                block = landed.at[group, sender]
                remote(block, block, o_send.at[group, 0], o_recv.at[group, sender], z, t).wait_recv()

            block = landed[group, sender].astype(f32)
            for step in range(props):
                out_ref[step, pl.ds(8 * group, live), pl.ds(at, piece)] = block[
                    8 * step : 8 * step + live
                ]

    def drain(group):
        def other(j):
            first_copy(group, j, z).wait_send()
            for stage, held in forwards():
                for at in held:
                    forward_copy(group, j, at, stage).wait_send()
            sum_copy(group, j, z).wait_send()
            hidden_copy(group, j, z).wait_send()

        each_other(other)
        for j in range(kv_size):
            for stage in range(stages):
                half_copy(group, stage, j).wait_send()

            @pl.when(jnp.logical_or(j != z, t != z))
            def _(j=j):
                final_copy(group, j).wait_send()


    token_load.wait()
    for group in range(groups):
        normalize(group)
        start_rows(group)
    fold_weights()
    for load in weight_loads:
        load.wait()
    key_load.wait()
    value_load.wait()
    own_part(0)
    fold(0)
    out_load.wait()
    for group in range(groups + 3):
        if group < groups:
            forward_rows(group)
            send_sums(group)
        if 0 < group < groups:
            own_part(group)
            fold(group)
        if 1 <= group <= groups:
            read(group - 1)
        if 2 <= group <= groups + 1:
            multiply(group - 2)
            for stage in range(stages):
                reduce(group - 2, stage)
        if group >= 3:
            finish(group - 3)
    for group in range(groups):
        drain(group)


def step(
    tokens, norm_gain, w_query, w_key, w_value, w_igate, w_fgate, igate_bias, fgate_bias, head_gain,
    w_out, state_matrix, state_norm, state_max, prior_keys, prior_values, prior_igate, prior_fgate,
    accepted, kv_size, tp_size,
):
    seqs, props, features = tokens.shape
    heads, key_size = state_matrix.shape[1:3]
    depth, width = w_query.shape
    out_width = w_out.shape[1]
    groups = -(-seqs // 8)
    rows = 8 * props
    stages = tp_size.bit_length() - 1
    piece = out_width // tp_size
    f32, bf16 = jnp.float32, jnp.bfloat16
    sem = pltpu.SemaphoreType.DMA
    hbm = pl.BlockSpec(memory_space=pl.ANY)
    vmem = pl.BlockSpec(memory_space=pltpu.VMEM)
    halves = []
    for stage in range(stages):
        halves += [pltpu.VMEM((groups, kv_size, rows, out_width >> (stage + 1)), bf16)] * 2
    by_step = (1, 0, 2)
    mixed, new_matrix, new_norm, new_max = pl.pallas_call(
        functools.partial(step_kernel, (kv_size, tp_size, seqs, props, heads)),
        out_shape=(
            jax.ShapeDtypeStruct((props, seqs, out_width), f32),
            pltpu.VMEM(state_matrix.shape, f32),
            jax.ShapeDtypeStruct(state_norm.shape, f32),
            jax.ShapeDtypeStruct((heads, seqs), f32),
        ),
        in_specs=[hbm, vmem, hbm, hbm, hbm, vmem, vmem, vmem, vmem, vmem, hbm, hbm, vmem, vmem]
        + [hbm, hbm, vmem, vmem, vmem],
        out_specs=(vmem, vmem, vmem, vmem),
        scratch_shapes=[
            pltpu.VMEM((props, seqs, features), bf16),
            pltpu.VMEM((groups, rows, features), bf16),
            pltpu.VMEM((kv_size, groups, rows, depth), bf16),
            pltpu.VMEM((depth, 3 * width), bf16),
            pltpu.VMEM((groups, rows, 3 * width), f32),
            pltpu.VMEM((rows, 3 * width), f32),
            pltpu.VMEM((kv_size, groups, rows, 3 * width), bf16),
            pltpu.VMEM((kv_size, groups, rows, 3 * width), bf16),
            pltpu.VMEM((2, groups, rows, 3 * width), bf16),
            pltpu.VMEM((props, seqs, width), bf16),
            pltpu.VMEM((props, seqs, width), bf16),
            pltpu.VMEM(state_matrix.shape, f32),
            pltpu.VMEM((groups, heads, key_size, 8 * key_size), bf16),
            pltpu.VMEM((2, 128, 128), f32),
            pltpu.VMEM((128, 128), f32),
            pltpu.VMEM((128, 128), f32),
            pltpu.VMEM((width, out_width), bf16),
            pltpu.VMEM((groups, kv_size, rows, width), bf16),
            pltpu.VMEM((groups, kv_size, rows, out_width), f32),
            pltpu.VMEM((groups, kv_size, rows, piece), bf16),
            pltpu.VMEM((groups, tp_size, rows, piece), bf16),
            *halves,
            sem((7,)),
            sem((groups,)),
            sem((groups, kv_size)),
            sem((groups, kv_size)),
            sem((groups, kv_size, tp_size, stages)),
            sem((groups, kv_size, tp_size)),
            sem((groups, kv_size)),
            sem((groups, kv_size)),
            sem((groups, 2)),
            sem((groups, kv_size)),
            sem((groups, kv_size)),
            sem((groups, stages, kv_size)),
            sem((groups, stages, kv_size)),
            sem((groups, kv_size)),
            sem((groups, tp_size)),
        ],
        compiler_params=pltpu.CompilerParams(
            collective_id=0, has_side_effects=True, vmem_limit_bytes=55 * 1024 * 1024
        ),
    )(
        tokens.transpose(by_step),
        norm_gain.reshape(-1, 128),
        w_query,
        w_key,
        w_value,
        w_igate.T,
        w_fgate.T,
        igate_bias[None, :],
        fgate_bias[None, :],
        head_gain.reshape(-1, key_size),
        w_out,
        state_matrix,
        state_norm,
        state_max.T,
        prior_keys.transpose(by_step),
        prior_values.transpose(by_step),
        prior_igate.transpose(1, 2, 0),
        prior_fgate.transpose(1, 2, 0),
        accepted[None, :],
    )
    return mixed.transpose(by_step), new_matrix, new_norm, new_max.T


def kernel_fits(kv_size, tp_size, tokens, w_query, w_out, state_matrix):
    seqs, props, width = tokens.shape
    heads, key_size, value_size = state_matrix.shape[1:]
    powers = kv_size == tp_size and 2 <= tp_size and tp_size & (tp_size - 1) == 0
    lanes = 128 * tp_size
    cut = (width // kv_size) % lanes == 0 and w_out.shape[1] % lanes == 0
    square = key_size == value_size == 128 and w_query.shape[1] == heads * key_size
    small = heads <= 8 and 8 * (props + 1) <= 128 and props % 2 == 0 and seqs <= 128
    return powers and cut and square and small


def reduce_tiles(partial, axis_name, axis):
    size = lax.psum(1, axis_name)
    shape = partial.shape
    split = partial.astype(jnp.bfloat16).reshape(
        shape[:axis] + (size, shape[axis] // size) + shape[axis + 1 :]
    )
    split = jnp.moveaxis(split, axis, 0)
    got = lax.all_to_all(split, axis_name, split_axis=0, concat_axis=0, tiled=True)
    return jnp.sum(got.astype(jnp.float32), axis=0)


def bf_dot(spec, left, right):
    return jnp.einsum(
        spec,
        left.astype(jnp.bfloat16),
        right.astype(jnp.bfloat16),
        preferred_element_type=jnp.float32,
    )


def heads_first(array, heads):
    seqs_n, props, width = array.shape
    return (
        array.astype(jnp.float32)
        .reshape(seqs_n, props, heads, width // heads)
        .transpose(0, 2, 1, 3)
    )


def fold_prior(matrix, normer, stabil, keys, values, in_pre, forget_pre, accepted):
    positions = jnp.arange(keys.shape[2], dtype=jnp.int32)
    active_mask = positions[None, None, :] < accepted[:, None, None]
    log_forget = jnp.where(active_mask, jax.nn.log_sigmoid(forget_pre), 0.0)
    in_gate = jnp.where(active_mask, in_pre, -1e30)
    cum_forget = jnp.cumsum(log_forget, axis=-1)
    total_forget = cum_forget[..., -1]
    weight_log = total_forget[..., None] - cum_forget + in_gate
    new_stabil = jnp.maximum(total_forget + stabil, jnp.max(weight_log, axis=-1))
    carry_scale = jnp.exp(total_forget + stabil - new_stabil)
    weighted_keys = keys * jnp.exp(weight_log - new_stabil[..., None])[..., None]
    new_matrix = carry_scale[..., None, None] * matrix + bf_dot(
        "bhtd,bhte->bhde", weighted_keys, values
    )
    new_normer = carry_scale[..., None] * normer + jnp.sum(weighted_keys, axis=2)
    return (new_matrix, new_normer, new_stabil)


def read_block(matrix, normer, stabil, query, keys, values, in_pre, forget_pre):
    props = query.shape[2]
    cum_forget = jnp.cumsum(jax.nn.log_sigmoid(forget_pre), axis=-1)
    causal = jnp.tril(jnp.ones((props, props), jnp.bool_))
    log_decay = jnp.where(
        causal, cum_forget[..., :, None] - cum_forget[..., None, :] + in_pre[..., None, :], -1e30
    )
    inter = cum_forget + stabil[..., None]
    row_max = jnp.maximum(inter, jnp.max(log_decay, axis=-1))
    inter_scale = jnp.exp(inter - row_max)
    scores = bf_dot("bhtd,bhud->bhtu", query, keys)
    scores = scores * jnp.exp(log_decay - row_max[..., None])
    numerator = inter_scale[..., None] * bf_dot(
        "bhtd,bhde->bhte", query, matrix
    )
    numerator = numerator + bf_dot(
        "bhtu,bhue->bhte", scores, values
    )
    denominator = inter_scale * jnp.sum(query * normer[:, :, None, :], axis=-1)
    denominator = denominator + jnp.sum(scores, axis=-1)
    return numerator / jnp.maximum(jnp.abs(denominator), jnp.exp(-row_max))[..., None]


def head_norm(cell, head_gain):
    seqs_n, heads, props, width = cell.shape
    scaled = cell * lax.rsqrt(jnp.mean(cell * cell, axis=-1, keepdims=True) + EPS)
    scaled = scaled.transpose(0, 2, 1, 3).reshape(seqs_n * props, heads * width)
    return (scaled * head_gain.astype(jnp.float32)).astype(jnp.bfloat16)


def body(
    tokens,
    norm_gain,
    w_query,
    w_key,
    w_value,
    w_igate,
    w_fgate,
    igate_bias,
    fgate_bias,
    head_gain,
    w_out,
    state_matrix,
    state_norm,
    state_max,
    prior_keys,
    prior_values,
    prior_igate,
    prior_fgate,
    accepted,
):
    kv_size, tp_size = lax.axis_size("kv"), lax.axis_size("tp")
    if kernel_fits(kv_size, tp_size, tokens, w_query, w_out, state_matrix):
        return step(
            tokens, norm_gain, w_query, w_key, w_value, w_igate, w_fgate, igate_bias, fgate_bias,
            head_gain, w_out, state_matrix, state_norm, state_max, prior_keys, prior_values,
            prior_igate, prior_fgate, accepted, kv_size, tp_size,
        )
    seq_count, props, width = tokens.shape
    local_heads = state_matrix.shape[1]
    key_size = state_matrix.shape[2]
    row_count = seq_count * props
    inputs = tokens.astype(jnp.float32)
    normed = inputs * lax.rsqrt(jnp.mean(inputs * inputs, axis=-1, keepdims=True) + EPS)
    normed_rows = (
        (normed * norm_gain.astype(jnp.float32)).astype(jnp.bfloat16).reshape(row_count, width)
    )
    query_width = w_query.shape[1]
    combined = jnp.concatenate([w_query, w_key, w_value], axis=1)
    received = lax.all_to_all(normed_rows, "kv", split_axis=1, concat_axis=0, tiled=True)
    summed = reduce_tiles(
        jnp.dot(received, combined, preferred_element_type=jnp.float32), "kv", 0
    )
    query_sum = summed[:, :query_width]
    key_sum = summed[:, query_width : 2 * query_width]
    value_sum = summed[:, 2 * query_width :]
    query = query_sum.astype(jnp.bfloat16).reshape(seq_count, props, -1)
    keys = key_sum.astype(jnp.bfloat16).reshape(seq_count, props, -1)
    values = value_sum.astype(jnp.bfloat16).reshape(seq_count, props, -1)
    in_pre = jnp.dot(normed_rows, w_igate, preferred_element_type=jnp.float32) + igate_bias
    forget_pre = jnp.dot(normed_rows, w_fgate, preferred_element_type=jnp.float32) + fgate_bias
    in_pre = in_pre.reshape(seq_count, props, local_heads).transpose(0, 2, 1)
    forget_pre = forget_pre.reshape(seq_count, props, local_heads).transpose(0, 2, 1)
    new_matrix, new_normer, new_stabil = fold_prior(
        state_matrix,
        state_norm,
        state_max,
        heads_first(prior_keys, local_heads) * key_size ** (-0.5),
        heads_first(prior_values, local_heads),
        prior_igate.transpose(0, 2, 1),
        prior_fgate.transpose(0, 2, 1),
        accepted,
    )
    cell = read_block(
        new_matrix,
        new_normer,
        new_stabil,
        heads_first(query, local_heads),
        heads_first(keys, local_heads) * key_size ** (-0.5),
        heads_first(values, local_heads),
        in_pre,
        forget_pre,
    )
    hidden = head_norm(cell, head_gain)
    partial_out = jnp.dot(
        hidden, lax.all_gather(w_out, "kv", axis=1, tiled=True), preferred_element_type=jnp.float32
    )
    mixed = reduce_tiles(partial_out, "tp", 1)
    return (mixed.reshape(seq_count, props, -1), new_matrix, new_normer, new_stabil)


def solution(mesh):
    return jax.shard_map(
        body,
        mesh=mesh,
        in_specs=(
            P(("grp", "kv"), None, None),
            P(),
            P("kv", "tp"),
            P("kv", "tp"),
            P("kv", "tp"),
            P(None, "tp"),
            P(None, "tp"),
            P("tp"),
            P("tp"),
            P("tp"),
            P("tp", "kv"),
            P(("grp", "kv"), "tp", None, None),
            P(("grp", "kv"), "tp", None),
            P(("grp", "kv"), "tp"),
            P(("grp", "kv"), None, "tp"),
            P(("grp", "kv"), None, "tp"),
            P(("grp", "kv"), None, "tp"),
            P(("grp", "kv"), None, "tp"),
            P(("grp", "kv")),
        ),
        out_specs=(
            P(("grp", "kv"), None, "tp"),
            P(("grp", "kv"), "tp", None, None),
            P(("grp", "kv"), "tp", None),
            P(("grp", "kv"), "tp"),
        ),
        check_vma=False,
    )
```
